32 devices in a mesh: sp: 8 (over z, x), tp: 4 (over y, core).
Axes of the slice: x: 2, y: 2, z: 4, core: 2. Of those that a mesh axis runs over, the one named last changes fastest.
Arguments:
- residual: bfloat16 [2048, 2048], P('sp', 'tp'), may hold values from -6 to 6
- queries: bfloat16 [2048, 1024], P('sp', 'tp'), may hold values from -5.5 to 5.5
- keys: bfloat16 [2048, 128], P('sp'), may hold values from -5.5 to 5.5
- values: bfloat16 [2048, 128], P('sp'), may hold values from -6 to 6
- documents: int32 [2048], P('sp'), may hold values from 0 to 3, never falling along the last dimension, each value on 1 to 1024 neighbouring positions
- sinks: float32 [16], P('tp'), may hold values from 1 to 6
- head_gain: float32 [1024], replicated, may hold values from 0.1 to 1.9
- out_weight: bfloat16 [1024, 2048], P(None, 'tp'), may hold values from -0.1875 to 0.1875
- norm_gain: float32 [2048], P('tp'), may hold values from 0.1 to 1.9
- norm_shift: float32 [2048], P('tp'), may hold values from -3 to 3
- routes: int32 [2048, 2], P('sp'), may hold values from 0 to 7, all different within a row; in each aligned block of 256 rows (0 to 255, 256 to 511, ...) at most 96 rows name the same one
- route_logits: float32 [2048, 2], P('sp'), may hold values from -150 to 150
- gate_weight: bfloat16 [8, 2048, 6144], P('sp', None, 'tp'), may hold values from -0.125 to 0.125
- up_weight: bfloat16 [8, 2048, 6144], P('sp', None, 'tp'), may hold values from -0.125 to 0.125
- down_weight: bfloat16 [8, 6144, 2048], P('sp', 'tp'), may hold values from -0.15625 to 0.15625
- final_gain: float32 [2048], P('tp'), may hold values from 0.1 to 1.9
- final_shift: float32 [2048], P('tp'), may hold values from -3 to 3
Outputs:
- layer_out: bfloat16 [2048, 2048], P('sp', 'tp')
The draws below stay inside these ranges and needn't reach their ends.
Inputs may be any that keep to these rules, and one draw needn't show every extreme that they name: `documents`: document numbers never fall along the sequence; each document has at least one position and at most 1024, and some document has exactly 1024. `routes`: each row names 2 different experts. In each aligned block of 256 rows (the rows of one index of sp) no expert is named by more than 96 rows, a bound that some block reaches.
All inputs are finite; a program needn't handle non-finite values.
Results may differ from the reference program's by a relative error of at most 0.014.
Values may be sent and summed in bfloat16 or wider, within the bound.
A program may use at most 128 MiB of HBM per device.

```python
import math
import jax
import jax.numpy as jnp
import numpy as np
from jax import lax

D = 2048
QUERY_HEADS = 16
KEY_VALUE_HEADS = 2
HEAD_SIZE = 64
FF = 6144
WINDOW_SIZE = 128
TOP = 2
TOK_SP = 256
PACKED_TOKENS = 2048
EXPERTS = 8
CAP = 96
DOCS = 4
DOC_MOST = 1024
N_SP = 8
N_TP = 4


def drawn_sample(key, salt, head_list):
    base = jax.random.truncated_normal(jax.random.fold_in(key, salt), -5.0, 5.0, (PACKED_TOKENS, head_list, HEAD_SIZE), jnp.float32)
    return base.reshape(PACKED_TOKENS, head_list * HEAD_SIZE).astype(jnp.bfloat16)


def draw_queries(key, part):
    return drawn_sample(key, 11, QUERY_HEADS)


def draw_keys(key, part):
    return drawn_sample(key, 13, KEY_VALUE_HEADS)


def draw_route_logits(key, part):
    logits = 1.5 * jax.random.truncated_normal(jax.random.fold_in(key, 17), -4.0, 4.0, (PACKED_TOKENS, TOP), jnp.float32)
    return logits


def block_scale(stream_key, extent, pieces, smallest, largest):
    level = 1.0
    for position, blocks in pieces:
        draws = jax.random.uniform(jax.random.fold_in(jax.random.fold_in(stream_key, 6), position), (blocks,), jnp.float32, smallest / len(pieces), largest / len(pieces))
        level = level * jnp.repeat(jnp.exp(draws), extent[position] // blocks).reshape((-1,) + (1,) * (len(extent) - 1 - position))
    return level


def profile(number_of, total, bound, lean):
    weights = [(1 << 20) // math.isqrt(standing ** lean) + 1 for standing in range(2, number_of + 1)]
    spare, counts = total - bound - (number_of - 1), [1] * (number_of - 1)
    while spare > 0:
        movable = [i for i in range(number_of - 1) if counts[i] < bound]
        mass, left = sum([weights[i] for i in movable]), spare
        for i in movable:
            addition = min(bound - counts[i], max(1, left * weights[i] // mass), spare)
            counts[i] = counts[i] + addition
            spare = spare - addition
    return np.array([bound] + counts)


def uneven_parts(stream_key, number_of, total, bound, skew):
    if number_of == 2:
        one = jax.random.randint(stream_key, (), max(1, total - bound), min(bound, total - 1) + 1)
        return jnp.stack([one, total - one])
    tallies = jnp.asarray(profile(number_of, total, bound, skew), jnp.int32)
    pairs = (number_of - 1) // 2
    giver, receiver = tallies[1:1 + 2 * pairs:2], tallies[2:2 + 2 * pairs:2]
    margin = jnp.minimum(giver - 1, bound - receiver)
    moved = jax.random.randint(jax.random.fold_in(stream_key, 1), (pairs,), 0, 1 << 20) % (margin + 1)
    tallies = tallies.at[1:1 + 2 * pairs:2].set(giver - moved).at[2:2 + 2 * pairs:2].set(receiver + moved)
    return tallies[jax.random.permutation(jax.random.fold_in(stream_key, 2), number_of)]


def deal_out(key, own, number, rows, number_of, top, reach, lean):
    order = jax.random.permutation(key, number_of)
    crowded, usual = shares(number_of, rows * top, reach, lean, True), shares(number_of, rows * top, reach, lean, False)
    places = jnp.arange(number_of)

    def named(lengths, turn):
        used = int((lengths > 0).sum())
        fixed = max(1, used // 4)
        passed = fixed + (places - fixed + turn * (used - fixed)) % max(1, number_of - fixed)
        return jnp.zeros((number_of,), jnp.int32).at[order[jnp.where(places < fixed, places, passed)]].set(jnp.asarray(lengths, jnp.int32))

    lengths = jnp.where(number % 4 == 0, named(crowded, number // 4), named(usual, number - number // 4 - 1))
    mixed = jax.random.permutation(jax.random.fold_in(own, 3), number_of)
    donor, receiver = mixed[0:number_of // 2 * 2:2], mixed[1:number_of // 2 * 2:2]
    room = jnp.minimum(lengths[donor] - 1, reach - lengths[receiver]) // 2
    room = jnp.where((donor == order[0]) | (receiver == order[0]) | (lengths[receiver] == 0), 0, jnp.maximum(room, 0))
    passed = jax.random.randint(jax.random.fold_in(own, 4), (number_of // 2,), 0, 1 << 20) % (room + 1)
    lengths = lengths.at[donor].add(-passed).at[receiver].add(passed)
    members = jnp.searchsorted(jnp.cumsum(lengths), jnp.arange(rows * top), side="right").astype(jnp.int32)
    table = members.reshape(top, rows).T
    table = table[jax.random.permutation(jax.random.fold_in(own, 1), rows)]
    turn = jax.random.randint(jax.random.fold_in(own, 2), (rows, 1), 0, top)
    return jnp.take_along_axis(table, (jnp.arange(top)[None, :] + turn) % top, axis=1)


def shares(count, total, most, skew, full):
    weights = [(1 << 20) // math.isqrt(grade ** skew) + 1 for grade in range(1, count + 1)]
    largest = most if full else min(most, max(-(-total // count), total * weights[0] // sum(weights)))
    least = 1 if total - largest >= count - 1 else 0
    given, spare = [largest] + [least] * (count - 1), total - largest - least * (count - 1)
    while spare > 0:
        movable = [i for i in range(1, count) if given[i] < largest] or [i for i in range(1, count) if given[i] < most]
        whole, left = sum([weights[i] for i in movable]), spare
        for i in movable:
            extra = min(most - given[i], max(1, left * weights[i] // whole), spare)
            given[i] = given[i] + extra
            spare = spare - extra
    return np.array(given)


def scatter_about(stream_key, extent, width, bound, split=(), held_as=jnp.bfloat16):
    entries = width * jax.random.normal(stream_key, extent, jnp.float32)
    if split:
        entries = entries * block_scale(stream_key, extent, split, -0.22, 0.18)
    return jnp.clip(entries, -bound, bound).astype(held_as)


def setup_inputs(seed: int = 0) -> dict:
    streams_of = jax.random.split(jax.random.key(seed), 18)
    residual = scatter_about(streams_of[0], (PACKED_TOKENS, D), 1.0, 6.0, ((0, 8), (1, 4)))
    queries = draw_queries(jax.random.fold_in(streams_of[17], 71), 0)
    keys = draw_keys(jax.random.fold_in(streams_of[17], 71), 0)
    values = scatter_about(streams_of[3], (PACKED_TOKENS, KEY_VALUE_HEADS * HEAD_SIZE), 1.0, 6.0, ((0, 8),))
    documents = jnp.searchsorted(jnp.cumsum(uneven_parts(streams_of[4], DOCS, PACKED_TOKENS, DOC_MOST, 1)), jnp.arange(PACKED_TOKENS), side="right").astype(jnp.int32)
    sinks = jnp.clip(1.0 + 5.0 * jax.random.uniform(streams_of[5], (QUERY_HEADS,), jnp.float32) ** block_scale(streams_of[5], (QUERY_HEADS,), ((0, 4),), -0.2, 0.2), 1.0, 6.0)
    head_gain = jnp.clip(1.0 + 0.18 * jax.random.normal(streams_of[6], (QUERY_HEADS * HEAD_SIZE,), jnp.float32), 0.1, 1.9)
    out_weight = scatter_about(streams_of[7], (QUERY_HEADS * HEAD_SIZE, D), (QUERY_HEADS * HEAD_SIZE) ** -0.5, 0.1875, ((1, 4),))
    norm_gain = jnp.clip(1.0 + 0.18 * jax.random.normal(streams_of[8], (D,), jnp.float32), 0.1, 1.9)
    norm_shift = scatter_about(streams_of[9], (D,), 0.5, 3.0, ((0, 4),), jnp.float32)
    routes_keys = jax.random.split(jax.random.fold_in(streams_of[10], 1), PACKED_TOKENS // TOK_SP)
    routes_turns = jax.random.permutation(jax.random.fold_in(streams_of[10], 3), PACKED_TOKENS // TOK_SP)
    routes = jax.vmap(lambda own, number: deal_out(jax.random.fold_in(streams_of[10], 2), own, number, TOK_SP, EXPERTS, TOP, CAP, 1))(routes_keys, routes_turns).reshape((PACKED_TOKENS, TOP))
    route_logits = draw_route_logits(jax.random.fold_in(streams_of[17], 71), 0)
    gate_weight = scatter_about(streams_of[12], (EXPERTS, D, FF), D ** -0.5, 0.125, ((0, 8), (2, 4)))
    up_weight = scatter_about(streams_of[13], (EXPERTS, D, FF), D ** -0.5, 0.125, ((0, 8), (2, 4)))
    down_weight = scatter_about(streams_of[14], (EXPERTS, FF, D), (FF // 4) ** -0.5, 0.15625, ((0, 8), (1, 4)))
    final_gain = jnp.clip(1.0 + 0.18 * jax.random.normal(streams_of[15], (D,), jnp.float32), 0.1, 1.9)
    final_shift = scatter_about(streams_of[16], (D,), 0.5, 3.0, ((0, 4),), jnp.float32)
    return {"residual": residual, "queries": queries, "keys": keys, "values": values, "documents": documents, "sinks": sinks, "head_gain": head_gain, "out_weight": out_weight, "norm_gain": norm_gain, "norm_shift": norm_shift, "routes": routes, "route_logits": route_logits, "gate_weight": gate_weight, "up_weight": up_weight, "down_weight": down_weight, "final_gain": final_gain, "final_shift": final_shift}


DEEP_ALPHA = 8.0 ** 0.25
NORM_EPS = 1e-05

def layer_norm(total, gain, shift):
    center = lax.optimization_barrier(jnp.sum(total, axis=-1, keepdims=True)) / D
    spread = lax.optimization_barrier(jnp.sum(total * total, axis=-1, keepdims=True)) / D - center * center
    return (total - center) * lax.rsqrt(spread + NORM_EPS) * gain + shift

def window_attention(queries, keys, values, documents, sinks):
    query_group = QUERY_HEADS // KEY_VALUE_HEADS
    padded_key_rows = jnp.concatenate([jnp.zeros((WINDOW_SIZE, KEY_VALUE_HEADS * HEAD_SIZE), jnp.bfloat16), keys], axis=0)
    padded_value_rows = jnp.concatenate([jnp.zeros((WINDOW_SIZE, KEY_VALUE_HEADS * HEAD_SIZE), jnp.bfloat16), values], axis=0)
    pad_docs = jnp.concatenate([jnp.full((WINDOW_SIZE,), -1, jnp.int32), documents.astype(jnp.int32)], axis=0)
    query_blocks = queries.reshape(PACKED_TOKENS // WINDOW_SIZE, WINDOW_SIZE, QUERY_HEADS, HEAD_SIZE)

    def one_block(inputs):
        query_block, index = inputs
        window_begin = (index * WINDOW_SIZE).astype(jnp.int32)
        key_tile_block = lax.dynamic_slice_in_dim(padded_key_rows, window_begin, 2 * WINDOW_SIZE, 0).reshape(2 * WINDOW_SIZE, KEY_VALUE_HEADS, HEAD_SIZE)
        value_tile_block = lax.dynamic_slice_in_dim(padded_value_rows, window_begin, 2 * WINDOW_SIZE, 0).reshape(2 * WINDOW_SIZE, KEY_VALUE_HEADS, HEAD_SIZE)
        key_docs = lax.dynamic_slice_in_dim(pad_docs, window_begin, 2 * WINDOW_SIZE, 0)
        query_docs = lax.dynamic_slice_in_dim(documents.astype(jnp.int32), window_begin, WINDOW_SIZE, 0)
        key_wide = jnp.repeat(key_tile_block, query_group, axis=1)
        value_wide = jnp.repeat(value_tile_block, query_group, axis=1)
        scores = jnp.einsum('qhd,khd->hqk', query_block.astype(jnp.float32), key_wide.astype(jnp.float32)) * HEAD_SIZE ** (-0.5)
        query_pos = window_begin + jnp.arange(WINDOW_SIZE, dtype=jnp.int32)
        key_pos = window_begin - WINDOW_SIZE + jnp.arange(2 * WINDOW_SIZE, dtype=jnp.int32)
        distance = query_pos[:, None] - key_pos[None, :]
        allowed = (distance >= 0) & (distance < WINDOW_SIZE) & (key_pos[None, :] >= 0) & (query_docs[:, None] == key_docs[None, :])
        scores = jnp.where(allowed[None], scores, -jnp.inf)
        sink_col = sinks.astype(jnp.float32)[:, None]
        top = jnp.maximum(lax.optimization_barrier(jnp.max(scores, axis=-1)), sink_col)
        expd = jnp.exp(scores - top[..., None])
        probs = (expd / (lax.optimization_barrier(jnp.sum(expd, axis=-1)) + jnp.exp(sink_col - top))[..., None]).astype(jnp.bfloat16)
        result = jnp.einsum('hqk,khd->qhd', probs.astype(jnp.float32), value_wide.astype(jnp.float32))
        return result.astype(jnp.bfloat16)
    blocks = lax.map(one_block, (query_blocks, jnp.arange(PACKED_TOKENS // WINDOW_SIZE, dtype=jnp.int32)))
    return blocks.reshape(PACKED_TOKENS, QUERY_HEADS * HEAD_SIZE)

def reference(residual, queries, keys, values, documents, sinks, head_gain, out_weight, norm_gain, norm_shift, routes, route_logits, gate_weight, up_weight, down_weight, final_gain, final_shift):
    attended = window_attention(queries, keys, values, documents, sinks).astype(jnp.float32)
    scaled = (attended * lax.rsqrt(lax.optimization_barrier(jnp.mean(attended * attended, axis=-1, keepdims=True)) + NORM_EPS) * head_gain).astype(jnp.bfloat16)
    mix = jnp.dot(scaled, out_weight, preferred_element_type=jnp.float32)
    first = DEEP_ALPHA * residual.astype(jnp.float32) + mix
    hidden = layer_norm(first, norm_gain, norm_shift)
    hidden_rows = hidden.astype(jnp.bfloat16)
    flat = routes.astype(jnp.int32).reshape(N_SP, TOK_SP * TOP)
    onehot = (flat[..., None] == jnp.arange(EXPERTS, dtype=jnp.int32)).astype(jnp.int32)
    rank = lax.optimization_barrier(jnp.sum(jnp.cumsum(onehot, axis=1) * onehot, axis=-1)) - 1
    source = jnp.arange(N_SP, dtype=jnp.int32)[:, None]
    place = ((flat * N_SP + source) * CAP + rank).astype(jnp.int32)
    owner = source * TOK_SP + jnp.arange(TOK_SP * TOP, dtype=jnp.int32)[None, :] // TOP
    table = jnp.full((EXPERTS * N_SP * CAP,), PACKED_TOKENS, jnp.int32).at[place.reshape(-1)].set(owner.reshape(-1).astype(jnp.int32))
    padded = jnp.concatenate([hidden_rows, jnp.zeros((1, D), jnp.bfloat16)], axis=0)

    def one_expert(inputs):
        index_rows, gate_w, up_w, down_w = inputs
        picked_rows = padded[index_rows]
        gate = jnp.dot(picked_rows, gate_w, preferred_element_type=jnp.float32)
        up_val = jnp.dot(picked_rows, up_w, preferred_element_type=jnp.float32)
        middle = (jax.nn.silu(gate) * up_val).astype(jnp.bfloat16)
        blocks = jnp.einsum('rjf,jfd->rjd', middle.reshape(-1, N_TP, FF // N_TP).astype(jnp.float32), down_w.reshape(N_TP, FF // N_TP, D).astype(jnp.float32))
        blocks = blocks.astype(jnp.bfloat16).astype(jnp.float32)
        return lax.optimization_barrier(jnp.sum(blocks, axis=1)).astype(jnp.bfloat16)
    outputs = lax.map(one_expert, (table.reshape(EXPERTS, N_SP * CAP), gate_weight, up_weight, down_weight))
    expert_out = outputs.reshape(EXPERTS * N_SP * CAP, D)[place.reshape(-1)].reshape(PACKED_TOKENS, TOP, D).astype(jnp.float32)
    share = jax.nn.softmax(route_logits.astype(jnp.float32), axis=-1)
    moe = lax.optimization_barrier(jnp.sum(share[:, :, None] * expert_out, axis=1))
    second = DEEP_ALPHA * hidden + moe
    return layer_norm(second, final_gain, final_shift).astype(jnp.bfloat16)
```

```python
import functools

import jax
import jax.numpy as jnp
from jax import lax
from jax.experimental import pallas as pl
from jax.experimental.pallas import tpu as pltpu
from jax.sharding import PartitionSpec as P

D = 2048
QUERY_HEADS = 16
KEY_VALUE_HEADS = 2
HEAD_SIZE = 64
WINDOW_SIZE = 128
TOP = 2


DEEP_ALPHA = 8.0**0.25
NORM_EPS = 1e-05


def shifted(block, axis, distance):
    devices = range(lax.axis_size(axis))
    route = [(i - distance, i) for i in devices if i - distance in devices]
    return lax.ppermute(block, axis, route)


def split_norm(total, gain, shift):
    totals = lax.psum((jnp.sum(total, axis=1), jnp.sum(total * total, axis=1)), "tp")
    center = totals[0] / D
    spread = totals[1] / D - center * center
    return (total - center[:, None]) * lax.rsqrt(spread + NORM_EPS)[:, None] * gain + shift


def swapped(index, step):
    partner, bit = index, 1
    while bit <= step:
        if step & bit:
            partner = partner + bit - 2 * bit * lax.rem(lax.div(index, bit), 2)
        bit *= 2
    return partner


def remote(source, target, sems, index, device):
    return pltpu.make_async_remote_copy(
        src_ref=source,
        dst_ref=target,
        send_sem=sems.at[(0,) + index],
        recv_sem=sems.at[(1,) + index],
        device_id=device,
        device_id_type=pl.DeviceIdType.MESH,
    )


def expert_kernel(
    n_sp,
    n_tp,
    group,
    rows_ref,
    gate_hbm,
    up_hbm,
    down_hbm,
    back_ref,
    gate_w,
    up_w,
    down_w,
    gathered,
    block,
    middle,
    parts,
    from_core,
    pair_sums,
    from_y,
    finished,
    landed,
    weight_sems,
    sp_sems,
    core_sems,
    y_sems,
    core_sum_sems,
    y_sum_sems,
    back_sems,
):
    f32 = jnp.float32
    n_y = n_tp // 2
    cap, width = rows_ref.shape[1:]
    ff = gate_w.shape[1]
    sp, tp = lax.axis_index("sp"), lax.axis_index("tp")
    y, core = lax.div(tp, 2), lax.rem(tp, 2)
    partner = {"sp": sp, "tp": tp + 1 - 2 * core}
    y_to = [lax.rem(y + j, n_y) for j in range(n_y)]
    y_from = [lax.rem(y + n_y - j, n_y) for j in range(n_y)]
    waiting = []

    weights = [
        pltpu.make_async_copy(hbm.at[0], vmem, weight_sems.at[i])
        for i, (hbm, vmem) in enumerate(
            ((gate_hbm, gate_w), (up_hbm, up_w), (down_hbm, down_w))
        )
    ]
    for copy in weights:
        copy.start()

    barrier = pltpu.get_barrier_semaphore()
    for k in range(1, n_sp):
        pl.semaphore_signal(
            barrier,
            inc=1,
            device_id={"sp": swapped(sp, k), "tp": tp},
            device_id_type=pl.DeviceIdType.MESH,
        )
    for j in range(1, n_tp):
        pl.semaphore_signal(
            barrier,
            inc=1,
            device_id={"sp": sp, "tp": lax.rem(tp + j, n_tp)},
            device_id_type=pl.DeviceIdType.MESH,
        )
    pl.semaphore_wait(barrier, n_sp + n_tp - 2)

    def launch(copy):
        copy.start()
        waiting.append(copy)
        return copy

    y_copies, core_copies = {}, {}

    def forward(k):
        if k:
            sp_copies[k].wait_recv()
        source = gathered.at[tp, k] if k else rows_ref.at[0]
        for j in range(1, n_y):
            device = {"sp": sp, "tp": y_to[j] * 2 + core}
            y_copies[j, k] = launch(
                remote(source, gathered.at[tp, k], y_sems, (j - 1, k), device)
            )
        core_copies[0, k] = launch(
            remote(source, gathered.at[tp, k], core_sems, (0, k), partner)
        )

    sp_copies = {}
    forward(0)
    for k in range(1, n_sp):
        device = {"sp": swapped(sp, k), "tp": tp}
        sp_copies[k] = launch(
            remote(rows_ref.at[k], gathered.at[tp, k], sp_sems, (k,), device)
        )
    gathered[tp, 0] = rows_ref[0]

    def relay(k):
        for j in range(1, n_y):
            y_copies[j, k].wait_recv()
            here = gathered.at[y_from[j] * 2 + core, k]
            core_copies[j, k] = launch(remote(here, here, core_sems, (j, k), partner))

    def arrive(k):
        for j in range(n_y):
            core_copies[j, k].wait_recv()

    def members(g):
        return range(g * group, (g + 1) * group)

    def span(g):
        return pl.ds(g * group, group)

    def compute(g):
        for t in range(n_tp):
            block[:, t * width : (t + 1) * width] = gathered[t, span(g)].reshape(
                group * cap, width
            )
        if g == 0:
            weights[0].wait()
            weights[1].wait()
        tile = next(size for size in (512, 384, 256, 128) if ff % size == 0)

        def hidden_tile(n, carry):
            columns = pl.ds(pl.multiple_of(n * tile, tile), tile)
            gate = jnp.dot(block[...], gate_w[:, columns], preferred_element_type=f32)
            up_val = jnp.dot(block[...], up_w[:, columns], preferred_element_type=f32)
            middle[:, columns] = (gate / (1.0 + jnp.exp(-gate)) * up_val).astype(jnp.bfloat16)
            return carry

        lax.fori_loop(0, ff // tile, hidden_tile, 0)
        if g == 0:
            weights[2].wait()

        def down_tile(n, carry):
            for c in range(2):
                columns = pl.ds(pl.multiple_of((2 * n + c) * width, width), width)
                share_out = jnp.dot(middle[...], down_w[:, columns], preferred_element_type=f32)
                parts[c, n, span(g)] = share_out.astype(jnp.bfloat16).reshape(group, cap, width)
            return carry

        lax.fori_loop(0, n_y, down_tile, 0)

    core_sum_copies, y_sum_copies = {}, {}

    def sum_core(g):
        core_sum_copies[g] = launch(
            remote(
                parts.at[1 - core, :, span(g)],
                from_core.at[:, span(g)],
                core_sum_sems,
                (g,),
                partner,
            )
        )

    def sum_y(g):
        core_sum_copies[g].wait_recv()
        for j in range(1, n_y):
            pair_sums[j - 1, span(g)] = (
                parts[core, y_to[j], span(g)].astype(f32)
                + from_core[y_to[j], span(g)].astype(f32)
            ).astype(jnp.bfloat16)
            y_sum_copies[j, g] = launch(
                remote(
                    pair_sums.at[j - 1, span(g)],
                    from_y.at[j - 1, span(g)],
                    y_sum_sems,
                    (j - 1, g),
                    {"sp": sp, "tp": y_to[j] * 2 + core},
                )
            )

    back_copies = []

    def send_back(g):
        total = parts[core, y, span(g)].astype(f32) + from_core[y, span(g)].astype(f32)
        for j in range(1, n_y):
            y_sum_copies[j, g].wait_recv()
            total = total + from_y[j - 1, span(g)].astype(f32)
        finished[span(g)] = total.astype(jnp.bfloat16)
        for k in members(g):
            if k:
                device = {"sp": swapped(sp, k), "tp": tp}
                back_copies.append(
                    launch(remote(finished.at[k], landed.at[k], back_sems, (k,), device))
                )

    groups = n_sp // group
    for k in members(0):
        if k:
            forward(k)
    for g in range(groups + 2):
        if g + 1 < groups:
            for k in members(g + 1):
                forward(k)
        if g < groups:
            for k in members(g):
                relay(k)
            for k in members(g):
                arrive(k)
            compute(g)
            sum_core(g)
        if 0 <= g - 1 < groups:
            sum_y(g - 1)
        if 0 <= g - 2 < groups:
            send_back(g - 2)
    back_ref[0] = finished[0]
    for k, copy in enumerate(back_copies, 1):
        copy.wait_recv()
        back_ref[k] = landed[k]
    for copy in waiting:
        copy.wait_send()


def expert_rows(outgoing, gate_weight, up_weight, down_weight):
    n_sp, n_tp = lax.axis_size("sp"), lax.axis_size("tp")
    _, cap, width = outgoing.shape
    _, depth, ff = gate_weight.shape
    group = 1
    while group * 2 <= n_sp and group * 2 * cap <= 256:
        group *= 2
    n_y = n_tp // 2
    half = jnp.bfloat16
    dma = pltpu.SemaphoreType.DMA
    return pl.pallas_call(
        functools.partial(expert_kernel, n_sp, n_tp, group),
        out_shape=jax.ShapeDtypeStruct(outgoing.shape, half),
        in_specs=[pl.BlockSpec(memory_space=pltpu.VMEM)]
        + [pl.BlockSpec(memory_space=pl.ANY)] * 3,
        out_specs=pl.BlockSpec(memory_space=pltpu.VMEM),
        scratch_shapes=[
            pltpu.VMEM((depth, ff), half),
            pltpu.VMEM((depth, ff), half),
            pltpu.VMEM((ff, depth), half),
            pltpu.VMEM((n_tp, n_sp, cap, width), half),
            pltpu.VMEM((group * cap, depth), half),
            pltpu.VMEM((group * cap, ff), half),
            pltpu.VMEM((2, n_y, n_sp, cap, width), half),
            pltpu.VMEM((n_y, n_sp, cap, width), half),
            pltpu.VMEM((n_y - 1, n_sp, cap, width), half),
            pltpu.VMEM((n_y - 1, n_sp, cap, width), half),
            pltpu.VMEM((n_sp, cap, width), half),
            pltpu.VMEM((n_sp, cap, width), half),
            dma((3,)),
            dma((2, n_sp)),
            dma((2, n_y, n_sp)),
            dma((2, n_y - 1, n_sp)),
            dma((2, n_sp // group)),
            dma((2, n_y - 1, n_sp // group)),
            dma((2, n_sp)),
        ],
        compiler_params=pltpu.CompilerParams(
            collective_id=0, has_side_effects=True, vmem_limit_bytes=60 * 1024 * 1024
        ),
        cost_estimate=pl.CostEstimate(
            flops=6 * n_sp * cap * depth * ff,
            bytes_accessed=6 * depth * ff,
            transcendentals=n_sp * cap * ff,
        ),
        name="experts",
    )(outgoing, gate_weight, up_weight, down_weight)


def local(
    residual,
    queries,
    keys,
    values,
    documents,
    sinks,
    head_gain,
    out_weight,
    norm_gain,
    norm_shift,
    routes,
    route_logits,
    gate_weight,
    up_weight,
    down_weight,
    final_gain,
    final_shift,
):
    tokens = queries.shape[0]
    head_list = sinks.shape[0]
    tail = shifted(
        jnp.concatenate(
            [
                keys[tokens - WINDOW_SIZE :],
                values[tokens - WINDOW_SIZE :],
                jnp.broadcast_to(
                    documents[tokens - WINDOW_SIZE :, None].astype(jnp.bfloat16),
                    (WINDOW_SIZE, 128),
                ),
            ],
            axis=1,
        ),
        "sp",
        1,
    )
    key_width = keys.shape[1]
    tails = (tail[:, :key_width], tail[:, key_width : 2 * key_width], tail[:, 2 * key_width])
    offset = lax.axis_index("sp") * tokens
    shared_key_head = lax.axis_index("tp") * head_list // (QUERY_HEADS // KEY_VALUE_HEADS)
    all_keys = jnp.concatenate([tails[0], keys], axis=0)
    all_values = jnp.concatenate([tails[1], values], axis=0)
    all_docs = jnp.concatenate([tails[2].astype(jnp.int32), documents], axis=0)
    key_head = lax.dynamic_slice_in_dim(all_keys, shared_key_head * HEAD_SIZE, HEAD_SIZE, 1)
    value_head = lax.dynamic_slice_in_dim(all_values, shared_key_head * HEAD_SIZE, HEAD_SIZE, 1)
    query_heads = queries.reshape(tokens, head_list, HEAD_SIZE)
    scores = jnp.einsum(
        "qhd,kd->hqk", query_heads, key_head, preferred_element_type=jnp.float32
    ) * HEAD_SIZE ** (-0.5)
    query_pos = offset + jnp.arange(tokens, dtype=jnp.int32)
    key_pos = offset - WINDOW_SIZE + jnp.arange(tokens + WINDOW_SIZE, dtype=jnp.int32)
    distance = query_pos[:, None] - key_pos[None, :]
    allowed = (
        (distance >= 0)
        & (distance < WINDOW_SIZE)
        & (key_pos[None, :] >= 0)
        & (documents[:, None] == all_docs[None, :])
    )
    scores = jnp.where(allowed[None], scores, -jnp.inf)
    sink_col = sinks[:, None]
    top = jnp.maximum(jnp.max(scores, axis=2), sink_col)
    expd = jnp.exp(scores - top[..., None])
    probs = (expd / (jnp.sum(expd, axis=2) + jnp.exp(sink_col - top))[..., None]).astype(
        jnp.bfloat16
    )
    attended = jnp.einsum("hqk,kd->qhd", probs, value_head, preferred_element_type=jnp.float32)
    attended = attended.astype(jnp.bfloat16).reshape(tokens, head_list * HEAD_SIZE)
    all_heads = lax.all_gather(attended, "tp", axis=1, tiled=True).astype(jnp.float32)
    scaled = (
        all_heads
        * lax.rsqrt(jnp.mean(all_heads * all_heads, axis=1, keepdims=True) + NORM_EPS)
        * head_gain
    ).astype(jnp.bfloat16)
    mix = jnp.dot(scaled, out_weight, preferred_element_type=jnp.float32)
    first = DEEP_ALPHA * residual.astype(jnp.float32) + mix
    hidden = split_norm(first, norm_gain, norm_shift)
    hidden_rows = hidden.astype(jnp.bfloat16)
    expert_count = lax.axis_size("sp")
    capacity = 3 * tokens * TOP // (2 * expert_count)
    slots = -(-capacity // 16) * 16
    chosen = routes[:, :, None] == jnp.arange(expert_count, dtype=jnp.int32)[None, None, :]
    named = jnp.any(chosen, axis=1).astype(jnp.bfloat16)
    earlier = jnp.tril(jnp.ones((tokens, tokens), jnp.bfloat16), -1)
    ahead = jnp.dot(earlier, named, preferred_element_type=jnp.float32)
    rank = jnp.sum(jnp.where(chosen, ahead[:, None, :], 0.0), axis=2).astype(jnp.int32)
    target = jnp.bitwise_xor(routes, lax.axis_index("sp")) * slots + rank
    places = jnp.arange(expert_count * slots, dtype=jnp.int32)[None, :]
    picks = [(target[:, r : r + 1] == places).astype(jnp.bfloat16) for r in range(TOP)]
    outgoing = lax.dot_general(
        sum(picks[1:], picks[0]),
        hidden_rows,
        (((0,), (0,)), ((), ())),
        preferred_element_type=jnp.float32,
    ).astype(jnp.bfloat16)
    returned = expert_rows(
        outgoing.reshape(expert_count, slots, -1), gate_weight, up_weight, down_weight
    ).reshape(expert_count * slots, -1)
    share = jax.nn.softmax(route_logits, axis=-1)
    moe = sum(
        share[:, r : r + 1] * jnp.dot(picks[r], returned, preferred_element_type=jnp.float32)
        for r in range(TOP)
    )
    second = DEEP_ALPHA * hidden + moe
    return split_norm(second, final_gain, final_shift).astype(jnp.bfloat16)


def solution(mesh):
    return jax.shard_map(
        local,
        mesh=mesh,
        in_specs=(
            P("sp", "tp"),
            P("sp", "tp"),
            P("sp", None),
            P("sp", None),
            P("sp"),
            P("tp"),
            P(),
            P(None, "tp"),
            P("tp"),
            P("tp"),
            P("sp", None),
            P("sp", None),
            P("sp", None, "tp"),
            P("sp", None, "tp"),
            P("sp", "tp", None),
            P("tp"),
            P("tp"),
        ),
        out_specs=P("sp", "tp"),
        check_vma=False,
    )
```
